32 devices in a mesh: ep: 8 (over z, x), tp: 4 (over y, core).
Axes of the slice: x: 2, y: 2, z: 4, core: 2. Of those that a mesh axis runs over, the one named last changes fastest.
Arguments:
- queries: bfloat16 [4096, 1024], P('ep', 'tp'), may hold values from -6 to 6
- sequence_keys: bfloat16 [4096, 1024], P('ep', 'tp'), may hold values from -6 to 6
- stream_content_vectors: bfloat16 [4096, 2048], P('ep', 'tp'), may hold values from -6 to 6
- output_gate_logits: bfloat16 [4096, 2048], P('ep', 'tp'), may hold values from -6 to 6
- retention_preactivation: bfloat16 [4096, 1024], P('ep', 'tp'), may hold values from -3 to 10
- additional_fade_bias: float32 [4096, 1024], P('ep', 'tp'), may hold values from -2.1 to 0
- attention_group_rescale: float32 [128], replicated, may hold values from 0.1 to 1.9
- output_projection: bfloat16 [2048, 2048], P(None, 'tp'), may hold values from -0.125 to 0.125
- expert_batch_tokens: bfloat16 [1024, 2048], P('ep'), may hold values from -6 to 6
- expert_norm_gain: float32 [2048], replicated, may hold values from 0.1 to 1.9
- routed_expert_index: int32 [1024, 4], P('ep'), may hold values from 0 to 7, all different within a row; in each aligned block of 128 rows (0 to 127, 128 to 255, ...) at most 128 rows name the same one
- routed_expert_weights: float32 [1024, 4], P('ep'), may hold values from 0.2 to 1.2
- expert_gate_matrix: bfloat16 [8, 2048, 2048], P('ep', None, 'tp'), may hold values from -0.125 to 0.125
- expert_up_matrix: bfloat16 [8, 2048, 2048], P('ep', None, 'tp'), may hold values from -0.125 to 0.125
- expert_down_matrix: bfloat16 [8, 2048, 2048], P('ep', None, 'tp'), may hold values from -0.125 to 0.125
- shared_gate_matrix: bfloat16 [2048, 2048], P(None, 'tp'), may hold values from -0.125 to 0.125
- shared_up_matrix: bfloat16 [2048, 2048], P(None, 'tp'), may hold values from -0.125 to 0.125
- shared_down_matrix: bfloat16 [2048, 2048], P(None, 'tp'), may hold values from -0.125 to 0.125
Outputs:
- mixer_out: bfloat16 [4096, 2048], P('ep', 'tp')
- specialist_blend: bfloat16 [1024, 2048], P('ep', 'tp')
The draws below stay inside these ranges and needn't reach their ends.
Inputs may be any that keep to these rules, and one draw needn't show every extreme that they name: `routed_expert_index`: each row names 4 different experts; among the rows of one index of ep no expert is named by more than 128 rows, a bound that some block reaches.
All inputs are finite; a program needn't handle non-finite values.
Results may differ from the reference program's by a relative error of at most 0.0069.
Values may be sent and summed in bfloat16 or wider, within the bound.
A program may use at most 64 MiB of HBM per device.

```python
import math
import jax
import jax.numpy as jnp
import numpy as np
from jax import lax

D = 2048
HEADS = 16
DK = 64
DV = 128
FF = 2048
SF = 2048
TOPK = 4
BLOCK = 64
SEQ_DEV = 512
TOK_B = 128
MIX = 2048
KW = 1024
TOKENS_A = 4096
TOKENS_B = 1024
EXPERTS = 8
CAP = 128
N_EP = 8


def draw_retention_preactivation(key, part):
    kind_key, fast_key, shift_key, noise_key = jax.random.split(jax.random.fold_in(key, 11), 4)
    slow_share = 0.5
    noise = jnp.clip(jax.random.normal(noise_key, (TOKENS_A, KW), jnp.float32) * 0.5, -1.5, 1.5)
    slow = jax.random.uniform(kind_key, (KW,), jnp.float32) < slow_share
    fast_base = jax.random.uniform(fast_key, (KW,), jnp.float32, -0.5, 1.0)
    slow_base = jnp.log(jnp.float32(TOKENS_A) / 8.0)
    base = jnp.where(slow, slow_base, fast_base)
    shift = jax.random.uniform(shift_key, (TOKENS_A // SEQ_DEV, 1), jnp.float32, -0.7, 0.7)
    shift = jnp.repeat(shift, SEQ_DEV, axis=0)
    return (base[None, :] + shift + noise).astype(jnp.bfloat16)


def draw_additional_fade_bias(key, part):
    place_key, depth_key = jax.random.split(jax.random.fold_in(key, 23))
    spots = jax.random.randint(place_key, (3,), 0, TOKENS_A)
    depth = jnp.log(jax.random.uniform(depth_key, (3, KW), jnp.float32, 0.5, 0.8))
    marks = (jnp.arange(TOKENS_A)[:, None] == spots[None, :]).astype(jnp.float32)
    return jnp.dot(marks, depth, precision=jax.lax.Precision.HIGHEST)


def block_levels(stream_key, dims, shards, least, top_value):
    loudness = 1.0
    for position, shards_of in shards:
        steps = jax.random.uniform(jax.random.fold_in(jax.random.fold_in(stream_key, 6), position), (shards_of,), jnp.float32, least / len(shards), top_value / len(shards))
        loudness = loudness * jnp.repeat(jnp.exp(steps), dims[position] // shards_of).reshape((-1,) + (1,) * (len(dims) - 1 - position))
    return loudness


def routed_block(own_key, own, number, rows, count, top, limit, skew):
    order = jax.random.permutation(own_key, count)
    crowded, ordinary = portions_of(count, rows * top, limit, skew, True), portions_of(count, rows * top, limit, skew, False)
    places = jnp.arange(count)

    def named(lengths, rotation):
        used = int((lengths > 0).sum())
        fixed = max(1, used // 4)
        shifted = fixed + (places - fixed + rotation * (used - fixed)) % max(1, count - fixed)
        return jnp.zeros((count,), jnp.int32).at[order[jnp.where(places < fixed, places, shifted)]].set(jnp.asarray(lengths, jnp.int32))

    lengths = jnp.where(number % 4 == 0, named(crowded, number // 4), named(ordinary, number - number // 4 - 1))
    mixed = jax.random.permutation(jax.random.fold_in(own, 3), count)
    giver, taker = mixed[0:count // 2 * 2:2], mixed[1:count // 2 * 2:2]
    room = jnp.minimum(lengths[giver] - 1, limit - lengths[taker]) // 2
    room = jnp.where((giver == order[0]) | (taker == order[0]) | (lengths[taker] == 0), 0, jnp.maximum(room, 0))
    shifted = jax.random.randint(jax.random.fold_in(own, 4), (count // 2,), 0, 1 << 20) % (room + 1)
    lengths = lengths.at[giver].add(-shifted).at[taker].add(shifted)
    members = jnp.searchsorted(jnp.cumsum(lengths), jnp.arange(rows * top), side="right").astype(jnp.int32)
    listing = members.reshape(top, rows).T
    listing = listing[jax.random.permutation(jax.random.fold_in(own, 1), rows)]
    rotation = jax.random.randint(jax.random.fold_in(own, 2), (rows, 1), 0, top)
    return jnp.take_along_axis(listing, (jnp.arange(top)[None, :] + rotation) % top, axis=1)


def portions_of(number_of, total, limit, slope, full):
    weights = [(1 << 20) // math.isqrt(standing ** slope) + 1 for standing in range(1, number_of + 1)]
    largest = limit if full else min(limit, max(-(-total // number_of), total * weights[0] // sum(weights)))
    least = 1 if total - largest >= number_of - 1 else 0
    given, rest = [largest] + [least] * (number_of - 1), total - largest - least * (number_of - 1)
    while rest > 0:
        candidates = [i for i in range(1, number_of) if given[i] < largest] or [i for i in range(1, number_of) if given[i] < limit]
        pool, budget = sum([weights[i] for i in candidates]), rest
        for i in candidates:
            addition = min(limit - given[i], max(1, budget * weights[i] // pool), rest)
            given[i] = given[i] + addition
            rest = rest - addition
    return np.array(given)


def scatter_about(own_key, dims, scale, most, shards=(), held_as=jnp.bfloat16):
    values = scale * jax.random.normal(own_key, dims, jnp.float32)
    if shards:
        values = values * block_levels(own_key, dims, shards, -0.22, 0.18)
    return jnp.clip(values, -most, most).astype(held_as)


def setup_inputs(seed: int = 0) -> dict:
    splits = jax.random.split(jax.random.key(seed), 19)
    queries = scatter_about(splits[0], (TOKENS_A, KW), 1.0, 6.0, ((0, 8), (1, 4)))
    sequence_keys = scatter_about(splits[1], (TOKENS_A, KW), 1.0, 6.0, ((0, 8), (1, 4)))
    stream_content_vectors = scatter_about(splits[2], (TOKENS_A, MIX), 1.0, 6.0, ((0, 8), (1, 4)))
    output_gate_logits = scatter_about(splits[3], (TOKENS_A, MIX), 1.0, 6.0, ((0, 8), (1, 4)))
    retention_preactivation = draw_retention_preactivation(jax.random.fold_in(splits[18], 71), 0)
    additional_fade_bias = draw_additional_fade_bias(jax.random.fold_in(splits[18], 71), 0)
    attention_group_rescale = jnp.clip(1.0 + 0.18 * jax.random.normal(splits[6], (DV,), jnp.float32), 0.1, 1.9)
    output_projection = scatter_about(splits[7], (MIX, D), MIX ** -0.5, 0.125, ((1, 4),))
    expert_batch_tokens = scatter_about(splits[8], (TOKENS_B, D), 1.0, 6.0, ((0, 8),))
    expert_norm_gain = jnp.clip(1.0 + 0.18 * jax.random.normal(splits[9], (D,), jnp.float32), 0.1, 1.9)
    routed_expert_index_keys = jax.random.split(jax.random.fold_in(splits[10], 1), TOKENS_B // TOK_B)
    routed_expert_index_turns = jax.random.permutation(jax.random.fold_in(splits[10], 3), TOKENS_B // TOK_B)
    routed_expert_index = jax.vmap(lambda own, number: routed_block(jax.random.fold_in(splits[10], 2), own, number, TOK_B, EXPERTS, TOPK, CAP, 2))(routed_expert_index_keys, routed_expert_index_turns).reshape((TOKENS_B, TOPK))
    routed_expert_weights = jnp.clip(0.2 + 1 * jax.random.uniform(splits[11], (TOKENS_B, TOPK), jnp.float32) ** block_levels(splits[11], (TOKENS_B, TOPK), ((0, 8),), -0.2, 0.2), 0.2, 1.2)
    expert_gate_matrix = scatter_about(splits[12], (EXPERTS, D, FF), D ** -0.5, 0.125, ((0, 8), (2, 4)))
    expert_up_matrix = scatter_about(splits[13], (EXPERTS, D, FF), D ** -0.5, 0.125, ((0, 8), (2, 4)))
    expert_down_matrix = scatter_about(splits[14], (EXPERTS, FF, D), FF ** -0.5, 0.125, ((0, 8), (2, 4)))
    shared_gate_matrix = scatter_about(splits[15], (D, SF), D ** -0.5, 0.125, ((1, 4),))
    shared_up_matrix = scatter_about(splits[16], (D, SF), D ** -0.5, 0.125, ((1, 4),))
    shared_down_matrix = scatter_about(splits[17], (SF, D), SF ** -0.5, 0.125, ((1, 4),))
    return {"queries": queries, "sequence_keys": sequence_keys, "stream_content_vectors": stream_content_vectors, "output_gate_logits": output_gate_logits, "retention_preactivation": retention_preactivation, "additional_fade_bias": additional_fade_bias, "attention_group_rescale": attention_group_rescale, "output_projection": output_projection, "expert_batch_tokens": expert_batch_tokens, "expert_norm_gain": expert_norm_gain, "routed_expert_index": routed_expert_index, "routed_expert_weights": routed_expert_weights, "expert_gate_matrix": expert_gate_matrix, "expert_up_matrix": expert_up_matrix, "expert_down_matrix": expert_down_matrix, "shared_gate_matrix": shared_gate_matrix, "shared_up_matrix": shared_up_matrix, "shared_down_matrix": shared_down_matrix}


eps_norm = 1e-06
switch_softness = 16.0
highest = lax.Precision.HIGHEST

def by_head(array, blocks, width):
    heads_here = array.shape[1] // width
    return array.astype(jnp.float32).reshape(blocks, BLOCK, heads_here, width).transpose(2, 0, 1, 3)

def carry_step(state, inputs):
    decay, update = inputs
    return (decay[..., None] * state + update, state)

def reference(queries, sequence_keys, stream_content_vectors, output_gate_logits, retention_preactivation, additional_fade_bias, attention_group_rescale, output_projection, expert_batch_tokens, expert_norm_gain, routed_expert_index, routed_expert_weights, expert_gate_matrix, expert_up_matrix, expert_down_matrix, shared_gate_matrix, shared_up_matrix, shared_down_matrix):
    blocks = TOKENS_A // BLOCK
    fade_exponent_rate = jax.nn.log_sigmoid(retention_preactivation.astype(jnp.float32)) / switch_softness + additional_fade_bias
    fade_exponent_rate = by_head(fade_exponent_rate, blocks, DK)
    inner = jnp.cumsum(fade_exponent_rate, axis=2)
    last = inner[:, :, -1:, :]
    query_f = by_head(queries, blocks, DK) * DK ** (-0.5)
    key_f = by_head(sequence_keys, blocks, DK)
    value_f = by_head(stream_content_vectors, blocks, DV)
    incoming_question = query_f * jnp.exp(inner)
    key_in = key_f * jnp.exp(-inner)
    causal = jnp.tril(jnp.ones((BLOCK, BLOCK), dtype=bool))
    scores = jnp.where(causal, jnp.einsum('hnid,hnjd->hnij', incoming_question, key_in, precision=highest), 0.0)
    mixed = jnp.einsum('hnij,hnje->hnie', scores, value_f, precision=highest)
    block_kv = jnp.einsum('hncd,hnce->hnde', key_f * jnp.exp(last - inner), value_f, precision=highest)
    block_decay = jnp.exp(last[:, :, 0, :])
    start_state = jnp.zeros((HEADS, DK, DV), jnp.float32)
    final_state, entering = lax.scan(carry_step, start_state, (jnp.moveaxis(block_decay, 1, 0), jnp.moveaxis(block_kv, 1, 0)))
    entering = jnp.moveaxis(entering, 0, 1)
    mixed = mixed + jnp.einsum('hncd,hnde->hnce', incoming_question, entering, precision=highest)
    mixed = mixed.transpose(1, 2, 0, 3).reshape(TOKENS_A, HEADS, DV)
    scale = lax.rsqrt(lax.optimization_barrier(jnp.mean(mixed * mixed, axis=-1, keepdims=True)) + eps_norm)
    gate_f = jax.nn.silu(output_gate_logits.astype(jnp.float32)).reshape(TOKENS_A, HEADS, DV)
    head_out = (mixed * scale * attention_group_rescale * gate_f).reshape(TOKENS_A, MIX).astype(jnp.bfloat16)
    mixer_out = jnp.dot(head_out, output_projection, preferred_element_type=jnp.float32).astype(jnp.bfloat16)
    flat = expert_batch_tokens.astype(jnp.float32)
    normed = (flat * lax.rsqrt(lax.optimization_barrier(jnp.mean(flat * flat, axis=-1, keepdims=True)) + eps_norm) * expert_norm_gain).astype(jnp.bfloat16)
    grouped = routed_expert_index.reshape(N_EP, TOK_B * TOPK)
    expert_ids = jnp.arange(EXPERTS, dtype=jnp.int32)
    onehot = (grouped[:, :, None] == expert_ids[None, None, :]).astype(jnp.int32)
    before = jnp.cumsum(onehot, axis=1).astype(jnp.int32) - onehot
    slot = lax.optimization_barrier(jnp.sum(before * onehot, axis=2)).astype(jnp.int32)
    source = jnp.broadcast_to(jnp.arange(N_EP, dtype=jnp.int32)[:, None], grouped.shape)
    owner = source * TOK_B + (jnp.arange(TOK_B * TOPK, dtype=jnp.int32) // TOPK)[None, :]
    table = jnp.full((EXPERTS, N_EP, CAP), TOKENS_B, dtype=jnp.int32).at[grouped, source, slot].set(owner)
    padded = jnp.concatenate([normed, jnp.zeros((1, D), jnp.bfloat16)], axis=0)

    def one_expert(inputs):
        slots, gate_w, up_w, down_w = inputs
        rows = padded[slots.reshape(-1)]
        gate_part = jnp.dot(rows, gate_w, preferred_element_type=jnp.float32)
        up_part = jnp.dot(rows, up_w, preferred_element_type=jnp.float32)
        hidden = (jax.nn.silu(gate_part) * up_part).astype(jnp.bfloat16)
        result = jnp.dot(hidden, down_w, preferred_element_type=jnp.float32).astype(jnp.bfloat16)
        return result.reshape(N_EP, CAP, D)
    results = lax.map(one_expert, (table, expert_gate_matrix, expert_up_matrix, expert_down_matrix))
    picked = results[grouped, source, slot].reshape(TOKENS_B, TOPK, D).astype(jnp.float32)
    routed = lax.optimization_barrier(jnp.sum(picked * routed_expert_weights[:, :, None], axis=1))
    shared_gate_part = jnp.dot(normed, shared_gate_matrix, preferred_element_type=jnp.float32)
    shared_up_part = jnp.dot(normed, shared_up_matrix, preferred_element_type=jnp.float32)
    shared_hidden = (jax.nn.silu(shared_gate_part) * shared_up_part).astype(jnp.bfloat16)
    shared_out = jnp.dot(shared_hidden, shared_down_matrix, preferred_element_type=jnp.float32)
    specialist_blend = (shared_out + routed).astype(jnp.bfloat16)
    return (mixer_out, specialist_blend)
```

```python
import jax
import jax.numpy as jnp
from jax import lax
from jax.experimental import pallas as pl
from jax.experimental.pallas import tpu as pltpu
from jax.sharding import PartitionSpec as P

DK = 64
DV = 128
BLOCK = 64
PAD = 16

eps_norm = 1e-06
switch_softness = 16.0
bf16 = jnp.bfloat16
f32 = jnp.float32
NT = (((1,), (1,)), ((), ()))
TN = (((0,), (0,)), ((), ()))


def silu(x):
    return x * jax.nn.sigmoid(x)


def scan_kernel(q_ref, k_ref, v_ref, r_ref, b_ref, mixed_ref, far_ref, left_ref, state_ref):
    width = q_ref.shape[1]
    heads = width // DK
    blocks = q_ref.shape[0] // BLOCK
    row = lax.broadcasted_iota(jnp.int32, (BLOCK, BLOCK), 0)
    col = lax.broadcasted_iota(jnp.int32, (BLOCK, BLOCK), 1)
    causal = row >= col
    tril = causal.astype(f32)
    state_ref[...] = jnp.zeros_like(state_ref)

    def turn(n, _):
        at = pl.ds(pl.multiple_of(n * BLOCK, BLOCK), BLOCK)
        r = r_ref[at, :].astype(f32)
        log_sig = jnp.minimum(r, 0.0) - jnp.log1p(jnp.exp(-jnp.abs(r)))
        rate = log_sig / switch_softness + b_ref[at, :]
        inner = jnp.dot(tril, rate, precision=lax.Precision.HIGHEST, preferred_element_type=f32)
        last = inner[BLOCK - 1 : BLOCK, :]
        q = q_ref[at, :].astype(f32) * DK**-0.5
        k = k_ref[at, :].astype(f32)
        q_in = q * jnp.exp(inner)
        q_b = q_in.astype(bf16)
        k_b = (k * jnp.exp(-inner)).astype(bf16)
        k_out = (k * jnp.exp(last - inner)).astype(bf16)
        prior = state_ref[DV : DV + 1, :]
        far_ref[at, :] = (q * jnp.exp(inner + prior)).astype(bf16)
        entering = state_ref[0:DV, :]
        entering_b = entering.astype(bf16)
        updates = []
        for h in range(heads):
            ks = slice(h * DK, (h + 1) * DK)
            vs = slice(h * DV, (h + 1) * DV)
            v = v_ref[at, vs]
            scores = lax.dot_general(q_b[:, ks], k_b[:, ks], NT, preferred_element_type=f32)
            scores = jnp.where(causal, scores, 0.0).astype(bf16)
            out = jnp.dot(scores, v, preferred_element_type=f32)
            out += lax.dot_general(q_b[:, ks], entering_b[:, ks], NT, preferred_element_type=f32)
            mixed_ref[at, vs] = out
            updates.append(lax.dot_general(v, k_out[:, ks], TN, preferred_element_type=f32))
        state_ref[0:DV, :] = entering * jnp.exp(last) + jnp.concatenate(updates, axis=1)
        state_ref[DV : DV + 1, :] = prior + last
        return 0

    lax.fori_loop(0, blocks, turn, 0)
    fade = state_ref[DV : DV + 8, :]
    high = fade.astype(bf16)
    low = (fade - high.astype(f32)).astype(bf16)
    left_ref[0:DV, :] = state_ref[0:DV, :].astype(bf16)
    left_ref[DV : DV + PAD, :] = jnp.concatenate([high, low], axis=0)


def finish_kernel(mixed_ref, far_ref, gate_ref, gain_ref, *refs):
    state_refs, out_ref = refs[:-1], refs[-1]
    width = far_ref.shape[1]
    heads = width // DK
    state = jnp.zeros((DV, width), f32)
    for ref in reversed(state_refs):
        fade = ref[DV : DV + PAD, :].astype(f32)
        state = jnp.exp(fade[0:1] + fade[8:9]) * state + ref[0:DV, :].astype(f32)
    state = state.astype(bf16)
    gain = gain_ref[...]
    for h in range(heads):
        ks = slice(h * DK, (h + 1) * DK)
        vs = slice(h * DV, (h + 1) * DV)
        m = mixed_ref[:, vs] + lax.dot_general(
            far_ref[:, ks], state[:, ks], NT, preferred_element_type=f32
        )
        scale = lax.rsqrt(jnp.mean(m * m, axis=-1, keepdims=True) + eps_norm)
        gate = silu(gate_ref[:, vs].astype(f32))
        out_ref[:, vs] = (m * scale * gain * gate).astype(bf16)


def vmem(count):
    return [pl.BlockSpec(memory_space=pltpu.VMEM)] * count


def scan_local(q, k, v, r, b):
    seq, width = q.shape
    return pl.pallas_call(
        scan_kernel,
        out_shape=(
            jax.ShapeDtypeStruct((seq, v.shape[1]), f32),
            jax.ShapeDtypeStruct((seq, width), bf16),
            jax.ShapeDtypeStruct((DV + PAD, width), bf16),
        ),
        in_specs=vmem(5),
        out_specs=tuple(vmem(3)),
        scratch_shapes=[pltpu.VMEM((DV + 8, width), f32)],
        cost_estimate=pl.CostEstimate(
            flops=2 * 10**9, bytes_accessed=3 * 2**20, transcendentals=10**6
        ),
        name="scan_local",
    )(q, k, v, r, b)


def finish(mixed, far, states, gate, gain):
    return pl.pallas_call(
        finish_kernel,
        out_shape=jax.ShapeDtypeStruct(mixed.shape, bf16),
        in_specs=vmem(4 + len(states)),
        out_specs=pl.BlockSpec(memory_space=pltpu.VMEM),
        cost_estimate=pl.CostEstimate(
            flops=10**9, bytes_accessed=3 * 2**20, transcendentals=10**6
        ),
        name="finish",
    )(mixed, far, gate, gain, *states)


def swish_product(gate_part, up_part):
    return (jax.nn.silu(gate_part) * up_part).astype(bf16)


def shifted(x, axis, step, wrap=True):
    n = lax.axis_size(axis)
    pairs = [(i, (i + step) % n) for i in range(n) if wrap or 0 <= i + step < n]
    return lax.ppermute(x, axis, pairs)


def gather_features(x):
    n = lax.axis_size("tp")
    width = x.shape[1]
    me = lax.axis_index("tp")
    held = [(me, x)]
    for step in range(1, n // 2):
        held.append((lax.rem(me + n - 2 * step, n), shifted(x, "tp", 2 * step)))
    pairs = [(i, i ^ 1) for i in range(n)]
    held += [(lane + 1 - 2 * lax.rem(lane, 2), lax.ppermute(p, "tp", pairs)) for lane, p in held]
    out = jnp.zeros((x.shape[0], n * width), x.dtype)
    for lane, piece in held:
        out = lax.dynamic_update_slice(out, piece, (0, lane * width))
    return out


def dot(a, b):
    return jnp.dot(a, b, preferred_element_type=f32)


def local(
    queries,
    sequence_keys,
    stream_content_vectors,
    output_gate_logits,
    retention_preactivation,
    additional_fade_bias,
    attention_group_rescale,
    output_projection,
    expert_batch_tokens,
    expert_norm_gain,
    routed_expert_index,
    routed_expert_weights,
    expert_gate_matrix,
    expert_up_matrix,
    expert_down_matrix,
    shared_gate_matrix,
    shared_up_matrix,
    shared_down_matrix,
):
    token_count, model_width = expert_batch_tokens.shape
    experts = lax.axis_size("ep")
    lanes = lax.axis_size("tp")
    share = model_width // lanes
    flat = expert_batch_tokens.astype(f32)
    normed = (
        flat
        * lax.rsqrt(jnp.mean(flat * flat, axis=-1, keepdims=True) + eps_norm)
        * expert_norm_gain
    ).astype(bf16)
    columns = lax.dynamic_slice_in_dim(normed, lax.axis_index("tp") * share, share, 1)
    arrived = [shifted(columns, "ep", d) for d in range(1, experts)]
    mixed, far, state = scan_local(
        queries,
        sequence_keys,
        stream_content_vectors,
        retention_preactivation,
        additional_fade_bias,
    )
    states = [shifted(state, "ep", d, wrap=False) for d in range(1, experts)]

    gate_w, up_w, down_w = expert_gate_matrix[0], expert_up_matrix[0], expert_down_matrix[0]
    middle = experts // 2 - 1
    groups = [range(1, middle + 1), range(middle + 1, experts)]
    shared_hidden = swish_product(dot(normed, shared_gate_matrix), dot(normed, shared_up_matrix))
    own_hidden = swish_product(dot(normed, gate_w), dot(normed, up_w))
    near = gather_features(jnp.concatenate([shared_hidden, own_hidden], axis=0))

    named = routed_expert_index[:, :, None] == jnp.arange(experts, dtype=jnp.int32)
    weights = jnp.sum(jnp.where(named, routed_expert_weights[:, :, None], 0.0), axis=1)
    here = lax.axis_index("ep")

    def weighted(result, step):
        expert = lax.rem(here + step, experts)
        return result.astype(f32) * lax.dynamic_slice_in_dim(weights, expert, 1, axis=1)

    hiddens = []
    for group in groups:
        rows = gather_features(jnp.concatenate([arrived[d - 1] for d in group], axis=0))
        hidden = swish_product(dot(rows, gate_w), dot(rows, up_w))
        hiddens.append(gather_features(hidden))

    head_out = finish(
        mixed, far, states, output_gate_logits, attention_group_rescale.reshape(1, DV)
    )
    heads_all = gather_features(head_out)
    total = dot(near[:token_count], shared_down_matrix)
    total += weighted(dot(near[token_count:], down_w).astype(bf16), 0)
    for group, hidden in zip(groups, hiddens):
        result = dot(hidden, down_w).astype(bf16).reshape(len(group), token_count, -1)
        for place, d in enumerate(group):
            total += weighted(shifted(result[place], "ep", -d), d)
    mixer_out = dot(heads_all, output_projection)
    return (mixer_out.astype(bf16), total.astype(bf16))


def solution(mesh):
    in_specs = (
        P("ep", "tp"),
        P("ep", "tp"),
        P("ep", "tp"),
        P("ep", "tp"),
        P("ep", "tp"),
        P("ep", "tp"),
        P(),
        P(None, "tp"),
        P("ep", None),
        P(),
        P("ep", None),
        P("ep", None),
        P("ep", None, "tp"),
        P("ep", None, "tp"),
        P("ep", None, "tp"),
        P(None, "tp"),
        P(None, "tp"),
        P(None, "tp"),
    )
    out_specs = (P("ep", "tp"), P("ep", "tp"))
    return jax.shard_map(local, mesh=mesh, in_specs=in_specs, out_specs=out_specs, check_vma=False)
```

```python
import functools

import jax
import jax.numpy as jnp
from jax import lax
from jax.experimental import pallas as pl
from jax.experimental.pallas import tpu as pltpu
from jax.sharding import PartitionSpec as P

DK = 64
DV = 128
BLOCK = 64
PAD = 16

eps_norm = 1e-06
switch_softness = 16.0
bf16 = jnp.bfloat16
f32 = jnp.float32
NT = (((1,), (1,)), ((), ()))
TN = (((0,), (0,)), ((), ()))


def silu(x):
    return x * jax.nn.sigmoid(x)


def scan_kernel(q_ref, k_ref, v_ref, r_ref, b_ref, mixed_ref, far_ref, left_ref, state_ref):
    width = q_ref.shape[1]
    heads = width // DK
    blocks = q_ref.shape[0] // BLOCK
    row = lax.broadcasted_iota(jnp.int32, (BLOCK, BLOCK), 0)
    col = lax.broadcasted_iota(jnp.int32, (BLOCK, BLOCK), 1)
    causal = row >= col
    tril = causal.astype(f32)
    state_ref[...] = jnp.zeros_like(state_ref)

    def turn(n, _):
        at = pl.ds(pl.multiple_of(n * BLOCK, BLOCK), BLOCK)
        r = r_ref[at, :].astype(f32)
        log_sig = jnp.minimum(r, 0.0) - jnp.log1p(jnp.exp(-jnp.abs(r)))
        rate = log_sig / switch_softness + b_ref[at, :]
        inner = jnp.dot(tril, rate, precision=lax.Precision.HIGHEST, preferred_element_type=f32)
        last = inner[BLOCK - 1 : BLOCK, :]
        q = q_ref[at, :].astype(f32) * DK**-0.5
        k = k_ref[at, :].astype(f32)
        q_in = q * jnp.exp(inner)
        q_b = q_in.astype(bf16)
        k_b = (k * jnp.exp(-inner)).astype(bf16)
        k_out = (k * jnp.exp(last - inner)).astype(bf16)
        prior = state_ref[DV : DV + 1, :]
        far_ref[at, :] = (q * jnp.exp(inner + prior)).astype(bf16)
        entering = state_ref[0:DV, :]
        entering_b = entering.astype(bf16)
        updates = []
        for h in range(heads):
            ks = slice(h * DK, (h + 1) * DK)
            vs = slice(h * DV, (h + 1) * DV)
            v = v_ref[at, vs]
            scores = lax.dot_general(q_b[:, ks], k_b[:, ks], NT, preferred_element_type=f32)
            scores = jnp.where(causal, scores, 0.0).astype(bf16)
            out = jnp.dot(scores, v, preferred_element_type=f32)
            out += lax.dot_general(q_b[:, ks], entering_b[:, ks], NT, preferred_element_type=f32)
            mixed_ref[at, vs] = out
            updates.append(lax.dot_general(v, k_out[:, ks], TN, preferred_element_type=f32))
        state_ref[0:DV, :] = entering * jnp.exp(last) + jnp.concatenate(updates, axis=1)
        state_ref[DV : DV + 1, :] = prior + last
        return 0

    lax.fori_loop(0, blocks, turn, 0)
    fade = state_ref[DV : DV + 8, :]
    high = fade.astype(bf16)
    low = (fade - high.astype(f32)).astype(bf16)
    left_ref[0:DV, :] = state_ref[0:DV, :].astype(bf16)
    left_ref[DV : DV + PAD, :] = jnp.concatenate([high, low], axis=0)


def finish_kernel(axis, mixed_ref, far_ref, gate_ref, gain_ref, states_ref, out_ref):
    me = lax.axis_index(axis)
    width = far_ref.shape[1]
    heads = width // DK
    state = jnp.zeros((DV, width), f32)
    for n in range(states_ref.shape[0] - 1):
        fade = states_ref[n, DV : DV + PAD, :].astype(f32)
        new = jnp.exp(fade[0:1] + fade[8:9]) * state + states_ref[n, 0:DV, :].astype(f32)
        state = jnp.where(n < me, new, state)
    state = state.astype(bf16)
    gain = gain_ref[...]
    for h in range(heads):
        ks = slice(h * DK, (h + 1) * DK)
        vs = slice(h * DV, (h + 1) * DV)
        m = mixed_ref[:, vs] + lax.dot_general(
            far_ref[:, ks], state[:, ks], NT, preferred_element_type=f32
        )
        scale = lax.rsqrt(jnp.mean(m * m, axis=-1, keepdims=True) + eps_norm)
        gate = silu(gate_ref[:, vs].astype(f32))
        out_ref[:, vs] = (m * scale * gain * gate).astype(bf16)


def vmem(count):
    return [pl.BlockSpec(memory_space=pltpu.VMEM)] * count


def scan_local(q, k, v, r, b):
    seq, width = q.shape
    return pl.pallas_call(
        scan_kernel,
        out_shape=(
            jax.ShapeDtypeStruct((seq, v.shape[1]), f32),
            jax.ShapeDtypeStruct((seq, width), bf16),
            jax.ShapeDtypeStruct((DV + PAD, width), bf16),
        ),
        in_specs=vmem(5),
        out_specs=tuple(vmem(3)),
        scratch_shapes=[pltpu.VMEM((DV + 8, width), f32)],
        cost_estimate=pl.CostEstimate(
            flops=2 * 10**9, bytes_accessed=3 * 2**20, transcendentals=10**6
        ),
        name="scan_local",
    )(q, k, v, r, b)


def finish(mixed, far, states, gate, gain):
    return pl.pallas_call(
        functools.partial(finish_kernel, "ep"),
        out_shape=jax.ShapeDtypeStruct(mixed.shape, bf16),
        in_specs=vmem(5),
        out_specs=pl.BlockSpec(memory_space=pltpu.VMEM),
        cost_estimate=pl.CostEstimate(
            flops=10**9, bytes_accessed=3 * 2**20, transcendentals=10**6
        ),
        name="finish",
    )(mixed, far, gate, gain, states)


def swish_product(gate_part, up_part):
    return (jax.nn.silu(gate_part) * up_part).astype(bf16)


def shifted(x, axis, step):
    n = lax.axis_size(axis)
    pairs = [(i, (i + step) % n) for i in range(n)]
    return lax.ppermute(x, axis, pairs)


def gather_features(x):
    n = lax.axis_size("tp")
    width = x.shape[1]
    me = lax.axis_index("tp")
    held = [(me, x)]
    for step in range(1, n // 2):
        held.append((lax.rem(me + n - 2 * step, n), shifted(x, "tp", 2 * step)))
    pairs = [(i, i ^ 1) for i in range(n)]
    held += [(lane + 1 - 2 * lax.rem(lane, 2), lax.ppermute(p, "tp", pairs)) for lane, p in held]
    out = jnp.zeros((x.shape[0], n * width), x.dtype)
    for lane, piece in held:
        out = lax.dynamic_update_slice(out, piece, (0, lane * width))
    return out


def dot(a, b):
    return jnp.dot(a, b, preferred_element_type=f32)


def local(
    queries,
    sequence_keys,
    stream_content_vectors,
    output_gate_logits,
    retention_preactivation,
    additional_fade_bias,
    attention_group_rescale,
    output_projection,
    expert_batch_tokens,
    expert_norm_gain,
    routed_expert_index,
    routed_expert_weights,
    expert_gate_matrix,
    expert_up_matrix,
    expert_down_matrix,
    shared_gate_matrix,
    shared_up_matrix,
    shared_down_matrix,
):
    token_count, model_width = expert_batch_tokens.shape
    experts = lax.axis_size("ep")
    lanes = lax.axis_size("tp")
    share = model_width // lanes
    flat = expert_batch_tokens.astype(f32)
    normed = (
        flat
        * lax.rsqrt(jnp.mean(flat * flat, axis=-1, keepdims=True) + eps_norm)
        * expert_norm_gain
    ).astype(bf16)
    columns = lax.dynamic_slice_in_dim(normed, lax.axis_index("tp") * share, share, 1)
    arrived = [shifted(columns, "ep", d) for d in range(1, experts)]
    mixed, far, state = scan_local(
        queries,
        sequence_keys,
        stream_content_vectors,
        retention_preactivation,
        additional_fade_bias,
    )

    gate_w, up_w, down_w = expert_gate_matrix[0], expert_up_matrix[0], expert_down_matrix[0]
    middle = experts // 2 - 1
    groups = [range(1, middle + 1), range(middle + 1, experts)]
    shared_hidden = swish_product(dot(normed, shared_gate_matrix), dot(normed, shared_up_matrix))
    own_hidden = swish_product(dot(normed, gate_w), dot(normed, up_w))
    near = gather_features(jnp.concatenate([shared_hidden, own_hidden], axis=0))

    named = routed_expert_index[:, :, None] == jnp.arange(experts, dtype=jnp.int32)
    weights = jnp.sum(jnp.where(named, routed_expert_weights[:, :, None], 0.0), axis=1)
    here = lax.axis_index("ep")

    def weighted(result, step):
        expert = lax.rem(here + step, experts)
        return result.astype(f32) * lax.dynamic_slice_in_dim(weights, expert, 1, axis=1)

    hiddens, gathered = [], []
    for group in groups:
        rows = gather_features(jnp.concatenate([arrived[d - 1] for d in group], axis=0))
        gathered.append(rows)
        hidden = swish_product(dot(rows, gate_w), dot(rows, up_w))
        hiddens.append(gather_features(hidden))

    state = lax.optimization_barrier((state, gathered[0]))[0]
    states = lax.all_to_all(
        jnp.broadcast_to(state, (experts,) + state.shape), "ep", split_axis=0, concat_axis=0
    )
    head_out = finish(
        mixed, far, states, output_gate_logits, attention_group_rescale.reshape(1, DV)
    )
    heads_all = gather_features(head_out)
    total = dot(near[:token_count], shared_down_matrix)
    total += weighted(dot(near[token_count:], down_w).astype(bf16), 0)
    for group, hidden in zip(groups, hiddens):
        result = dot(hidden, down_w).astype(bf16).reshape(len(group), token_count, -1)
        for place, d in enumerate(group):
            total += weighted(shifted(result[place], "ep", -d), d)
    mixer_out = dot(heads_all, output_projection)
    return (mixer_out.astype(bf16), total.astype(bf16))


def solution(mesh):
    in_specs = (
        P("ep", "tp"),
        P("ep", "tp"),
        P("ep", "tp"),
        P("ep", "tp"),
        P("ep", "tp"),
        P("ep", "tp"),
        P(),
        P(None, "tp"),
        P("ep", None),
        P(),
        P("ep", None),
        P("ep", None),
        P("ep", None, "tp"),
        P("ep", None, "tp"),
        P("ep", None, "tp"),
        P(None, "tp"),
        P(None, "tp"),
        P(None, "tp"),
    )
    out_specs = (P("ep", "tp"), P("ep", "tp"))
    return jax.shard_map(local, mesh=mesh, in_specs=in_specs, out_specs=out_specs, check_vma=False)
```
